32 devices in a mesh: ep: 8 (over z, x), tp: 4 (over y, core).
Axes of the slice: x: 2, y: 2, z: 4, core: 2. Of those that a mesh axis runs over, the one named last changes fastest.
Arguments:
- tokens: bfloat16 [1024, 2048], P('ep'), may hold values from -6 to 6
- routes: int32 [1024, 2], P('ep'), may hold values from 0 to 7, all different within a row; in each aligned block of 128 rows (0 to 127, 128 to 255, ...) at most 36 rows name the same one
- route_gates: float32 [1024, 2], P('ep'), may hold values from 0.1 to 2
- cotangent: bfloat16 [1024, 2048], P('ep'), may hold values from -40 to 40
- w_gate: bfloat16 [8, 2048, 1536], P('ep', None, 'tp'), may hold values from -0.125 to 0.125
- w_up: bfloat16 [8, 2048, 1536], P('ep', None, 'tp'), may hold values from -0.125 to 0.125
- w_down: bfloat16 [8, 1536, 2048], P('ep', 'tp'), may hold values from -0.15625 to 0.15625
- s_gate: bfloat16 [2048, 1536], P(None, 'tp'), may hold values from -0.125 to 0.125
- s_up: bfloat16 [2048, 1536], P(None, 'tp'), may hold values from -0.125 to 0.125
- s_down: bfloat16 [1536, 2048], P('tp'), may hold values from -0.15625 to 0.15625
Outputs:
- token_grad: bfloat16 [1024, 2048], P('ep', 'tp')
- gate_grad: float32 [1024, 2], P('ep')
- grad_gate: float32 [8, 2048, 1536], P('ep', None, 'tp')
- grad_up: float32 [8, 2048, 1536], P('ep', None, 'tp')
- grad_down: float32 [8, 1536, 2048], P('ep', 'tp')
- grad_shared: float32 [1536, 2048], P(('tp', 'ep'))
- norm_in: float32 [8, 2, 2048], P('ep')
- norm_down: float32 [8, 1536], P('ep', 'tp')
- norm_shared: float32 [1536], P(('tp', 'ep'))
The draws below stay inside these ranges and needn't reach their ends.
Inputs may be any that keep to these rules, and one draw needn't show every extreme that they name: `routes`: within the rows of one index of ep no expert is named by more than 36 assignments, a bound that some block reaches.
All inputs are finite; a program needn't handle non-finite values.
Results may differ from the reference program's by a relative error of at most 0.0095.
Values may be sent and summed in bfloat16 or wider, within the bound.
A program may use at most 64 MiB of HBM per device.

```python
import math
import jax
import jax.numpy as jnp
import numpy as np
from jax import lax

D = 2048
FF = 1536
SHARED = 1536
TOP_K = 2
TOK_DEV = 128
EXPERTS = 8
CAP = 36
ROWS = 288
TOKENS = 1024
N_EP = 8
N_TP = 4


def draw_cotangent(key, part):
    first = jax.random.fold_in(key, 11)
    second = jax.random.fold_in(key, 12)
    third = jax.random.fold_in(key, 13)
    values = jax.random.normal(first, (TOKENS, D), jnp.float32)
    column_scale = jnp.exp(jax.random.uniform(third, (1, D), jnp.float32, math.log(0.3), math.log(3.0)))
    row_scale = jnp.exp(jax.random.uniform(second, (TOKENS, 1), jnp.float32, math.log(0.3), math.log(3.0)))
    values = jnp.clip(values, -5.0, 5.0)
    return (0.3 * values * row_scale * column_scale).astype(jnp.bfloat16)


def shard_levels(own_key, dims, shards, least, largest):
    def one(dim, blocks):
        steps = jax.random.uniform(jax.random.fold_in(jax.random.fold_in(own_key, 6), dim), (blocks,), jnp.float32, least / len(shards), largest / len(shards))
        return jnp.repeat(jnp.exp(steps), dims[dim] // blocks).reshape((-1,) + (1,) * (len(dims) - dim - 1))

    gain = one(*shards[0])
    for cut in shards[1:]:
        gain = gain * one(*cut)
    return gain


def routed_block(rng, own, number, rows, amount, top, bound, slope):
    order = jax.random.permutation(rng, amount)
    crowded, ordinary = portions_of(amount, rows * top, bound, slope, True), portions_of(amount, rows * top, bound, slope, False)
    places = jnp.arange(amount)

    def named(sizes, turn):
        used = int((sizes > 0).sum())
        fixed = max(1, used // 4)
        shifted = fixed + (places - fixed + turn * (used - fixed)) % max(1, amount - fixed)
        return jnp.zeros((amount,), jnp.int32).at[order[jnp.where(places < fixed, places, shifted)]].set(jnp.asarray(sizes, jnp.int32))

    sizes = jnp.where(number % 4 == 0, named(crowded, number // 4), named(ordinary, number - number // 4 - 1))
    mixed = jax.random.permutation(jax.random.fold_in(own, 3), amount)
    donor, taker = mixed[0:amount // 2 * 2:2], mixed[1:amount // 2 * 2:2]
    slack = jnp.minimum(sizes[donor] - 1, bound - sizes[taker]) // 2
    slack = jnp.where((donor == order[0]) | (taker == order[0]) | (sizes[taker] == 0), 0, jnp.maximum(slack, 0))
    shifted = jax.random.randint(jax.random.fold_in(own, 4), (amount // 2,), 0, 1 << 20) % (slack + 1)
    sizes = sizes.at[donor].add(-shifted).at[taker].add(shifted)
    labels = jnp.searchsorted(jnp.cumsum(sizes), jnp.arange(rows * top), side="right").astype(jnp.int32)
    listing = labels.reshape(top, rows).T
    listing = listing[jax.random.permutation(jax.random.fold_in(own, 1), rows)]
    turn = jax.random.randint(jax.random.fold_in(own, 2), (rows, 1), 0, top)
    return jnp.take_along_axis(listing, (jnp.arange(top)[None, :] + turn) % top, axis=1)


def portions_of(number_of, total, reach, lean, full):
    portions = [(1 << 20) // math.isqrt(rank ** lean) + 1 for rank in range(1, number_of + 1)]
    largest = reach if full else min(reach, max(-(-total // number_of), total * portions[0] // sum(portions)))
    least = 1 if total - largest >= number_of - 1 else 0
    given, surplus = [largest] + [least] * (number_of - 1), total - largest - least * (number_of - 1)
    while surplus > 0:
        movable = [i for i in range(1, number_of) if given[i] < largest] or [i for i in range(1, number_of) if given[i] < reach]
        pool, budget = sum([portions[i] for i in movable]), surplus
        for i in movable:
            addition = min(reach - given[i], max(1, budget * portions[i] // pool), surplus)
            given[i] = given[i] + addition
            surplus = surplus - addition
    return np.array(given)


def centred(stream_key, shape, scale, bound, shards=(), kind=jnp.bfloat16):
    drawn = jax.random.normal(stream_key, shape, jnp.float32) * scale
    if len(shards) > 0:
        drawn = shard_levels(stream_key, shape, shards, -0.22, 0.18) * drawn
    return jnp.clip(drawn, min=-bound, max=bound).astype(kind)


def setup_inputs(seed: int = 0) -> dict:
    arg_keys = jax.random.split(jax.random.key(seed), 11)
    tokens = centred(arg_keys[0], (TOKENS, D), 1.0, 6.0, ((0, 8),))
    routes_keys = jax.random.split(jax.random.fold_in(arg_keys[1], 1), TOKENS // TOK_DEV)
    routes_turns = jax.random.permutation(jax.random.fold_in(arg_keys[1], 3), TOKENS // TOK_DEV)
    routes = jax.vmap(lambda own, number: routed_block(jax.random.fold_in(arg_keys[1], 2), own, number, TOK_DEV, EXPERTS, TOP_K, CAP, 1))(routes_keys, routes_turns).reshape((TOKENS, TOP_K))
    route_gates = jnp.clip(jnp.exp(math.log(2.0) - 2.9957323 * jax.random.uniform(arg_keys[2], (TOKENS, TOP_K), jnp.float32) ** shard_levels(arg_keys[2], (TOKENS, TOP_K), ((0, 8),), -0.2, 0.2)), 0.1, 2.0)
    cotangent = draw_cotangent(jax.random.fold_in(arg_keys[10], 71), 0)
    w_gate = centred(arg_keys[4], (EXPERTS, D, FF), D ** -0.5, 0.125, ((0, 8), (2, 4)))
    w_up = centred(arg_keys[5], (EXPERTS, D, FF), D ** -0.5, 0.125, ((0, 8), (2, 4)))
    w_down = centred(arg_keys[6], (EXPERTS, FF, D), FF ** -0.5, 0.15625, ((0, 8), (1, 4)))
    s_gate = centred(arg_keys[7], (D, SHARED), D ** -0.5, 0.125, ((1, 4),))
    s_up = centred(arg_keys[8], (D, SHARED), D ** -0.5, 0.125, ((1, 4),))
    s_down = centred(arg_keys[9], (SHARED, D), SHARED ** -0.5, 0.15625, ((0, 4),))
    return {"tokens": tokens, "routes": routes, "route_gates": route_gates, "cotangent": cotangent, "w_gate": w_gate, "w_up": w_up, "w_down": w_down, "s_gate": s_gate, "s_up": s_up, "s_down": s_down}


def slot_table(routes):
    chosen = routes.reshape(N_EP, TOK_DEV * TOP_K)
    expert_ids = jnp.arange(EXPERTS, dtype=jnp.int32)
    one_hot = (chosen[:, :, None] == expert_ids[None, None, :]).astype(jnp.int32)
    ranks = jnp.sum((jnp.cumsum(one_hot, axis=1) - one_hot) * one_hot, axis=2)
    source = jnp.arange(N_EP, dtype=jnp.int32)[:, None]
    slot_of = chosen * ROWS + source * CAP + ranks
    return slot_of.reshape(TOKENS * TOP_K).astype(jnp.int32)


def block_sum(d_gate, d_up, gate_weight, up_weight):
    block_width = gate_weight.shape[1] // N_TP
    running = jnp.zeros((d_gate.shape[0], gate_weight.shape[0]), jnp.float32)
    for block_index in range(N_TP):
        lower = block_index * block_width
        upper = lower + block_width
        block_term = jnp.dot(d_gate[:, lower:upper], gate_weight[:, lower:upper].T, preferred_element_type=jnp.float32)
        block_term = block_term + jnp.dot(d_up[:, lower:upper], up_weight[:, lower:upper].T, preferred_element_type=jnp.float32)
        rounded = lax.optimization_barrier(block_term.astype(jnp.bfloat16))
        running = running + rounded.astype(jnp.float32)
    return running


def swiglu_back(rows_x, rows_c, gate_weight, up_weight, down_weight):
    pre_gate = jnp.dot(rows_x, gate_weight, preferred_element_type=jnp.float32)
    pre_up = jnp.dot(rows_x, up_weight, preferred_element_type=jnp.float32)
    sigmoid_gate = jax.nn.sigmoid(pre_gate)
    activated = pre_gate * sigmoid_gate
    hidden = (activated * pre_up).astype(jnp.bfloat16)
    hidden_grad = jnp.dot(rows_c, down_weight.T, preferred_element_type=jnp.float32)
    d_gate = (hidden_grad * pre_up * sigmoid_gate * (1.0 + pre_gate * (1.0 - sigmoid_gate))).astype(jnp.bfloat16)
    d_up = (hidden_grad * activated).astype(jnp.bfloat16)
    return hidden, hidden_grad, d_gate, d_up


def expert_back(args):
    rows_x, rows_c, gate_weight, up_weight, down_weight = args
    hidden, hidden_grad, d_gate, d_up = swiglu_back(rows_x, rows_c, gate_weight, up_weight, down_weight)
    gate_dot = jnp.sum(hidden.astype(jnp.float32) * hidden_grad, axis=1).astype(jnp.bfloat16)
    grad_gate = jnp.dot(rows_x.T, d_gate, preferred_element_type=jnp.float32)
    grad_up = jnp.dot(rows_x.T, d_up, preferred_element_type=jnp.float32)
    grad_down = jnp.dot(hidden.T, rows_c, preferred_element_type=jnp.float32)
    slot_grad = block_sum(d_gate, d_up, gate_weight, up_weight)
    return grad_gate, grad_up, grad_down, slot_grad, gate_dot


def reference(tokens, routes, route_gates, cotangent, w_gate, w_up, w_down, s_gate, s_up, s_down):
    slot_of = slot_table(routes)
    token_of = (jnp.arange(TOKENS * TOP_K, dtype=jnp.int32) // TOP_K).astype(jnp.int32)
    row_token = jnp.full((EXPERTS * ROWS,), TOKENS, jnp.int32).at[slot_of].set(token_of)
    row_gate = jnp.zeros((EXPERTS * ROWS,), jnp.float32).at[slot_of].set(route_gates.reshape(TOKENS * TOP_K))
    padded_x = jnp.concatenate([tokens, jnp.zeros((1, D), jnp.bfloat16)], axis=0)
    padded_c = jnp.concatenate([cotangent, jnp.zeros((1, D), jnp.bfloat16)], axis=0)
    slot_x = padded_x[row_token].reshape(EXPERTS, ROWS, D)
    slot_c = (row_gate[:, None] * padded_c[row_token].astype(jnp.float32)).astype(jnp.bfloat16).reshape(EXPERTS, ROWS, D)
    grad_gate, grad_up, grad_down, slot_grad, gate_dot = lax.map(expert_back, (slot_x, slot_c, w_gate, w_up, w_down))
    routed = jax.ops.segment_sum(slot_grad.reshape(EXPERTS * ROWS, D), row_token, num_segments=TOKENS + 1)[:TOKENS]
    gate_grad = gate_dot.reshape(EXPERTS * ROWS)[slot_of].reshape(TOKENS, TOP_K).astype(jnp.float32) / route_gates
    s_hidden, s_hidden_grad, s_d_gate, s_d_up = swiglu_back(tokens, cotangent, s_gate, s_up, s_down)
    grad_shared = jnp.dot(s_hidden.T, cotangent, preferred_element_type=jnp.float32)
    shared_back = block_sum(s_d_gate, s_d_up, s_gate, s_up)
    token_grad = (shared_back + routed).astype(jnp.bfloat16)
    norm_in = jnp.stack([jnp.mean(grad_gate ** 2, axis=2), jnp.mean(grad_up ** 2, axis=2)], axis=1)
    norm_down = jnp.mean(grad_down ** 2, axis=2)
    norm_shared = jnp.mean(grad_shared ** 2, axis=1)
    return (token_grad, gate_grad, grad_gate, grad_up, grad_down, grad_shared, norm_in, norm_down, norm_shared)
```

```python
import functools

import jax
import jax.numpy as jnp
from jax import lax
from jax.experimental import pallas as pl
from jax.experimental.pallas import tpu as pltpu
from jax.sharding import PartitionSpec as P

MESH = pl.DeviceIdType.MESH
CORES = 2
BF = jnp.bfloat16
F32 = jnp.float32


def dot(a, b, ca=1, cb=0):
    return lax.dot_general(a, b, (((ca,), (cb,)), ((), ())), preferred_element_type=F32)


def activations(pre_gate, pre_up, hidden_grad):
    sig = jax.nn.sigmoid(pre_gate)
    act = pre_gate * sig
    hidden = (act * pre_up).astype(BF)
    d_gate = (hidden_grad * pre_up * sig * (1.0 + pre_gate * (1.0 - sig))).astype(BF)
    d_up = (hidden_grad * act).astype(BF)
    return hidden, d_gate, d_up


def body(
    ep, tp, cap_pad,
    slot_row, slot_col, gates, tokens, cot, wg_h, wu_h, wd_h, sg_h, su_h, sd_h,
    token_out, gate_out, shared_out, norm_in_out, norm_down_out, norm_sh_out,
    x_out, c_out, hid_out, dg_out, du_out,
    wg, wu, wd, sg, su, sd, send, rx, acc, prod, term, term_rx,
    part_a, part_own, recv_a, part_b, recv_b, back_tx, back_rx, shared_tot,
    gpart, grecv, gsend, gback, sq, sq_rx,
    w_sem, out_sem, d1_s, d1_r, d2_s, d2_r, pass_s, rs_s, rs_r, ra_s, ra_r, rb_s, rb_r,
    bk_s, bk_r, g_s, g_r, gb_s, gb_r, q_s, q_r,
):
    me = lax.axis_index("ep")
    j = lax.axis_index("tp")
    core = lax.rem(j, CORES)
    y = lax.div(j, CORES)
    mate = j + 1 - 2 * core
    ny = tp // CORES
    rows = ep * cap_pad
    tok, width = tokens.shape
    share = width // tp
    top = slot_row.shape[0]
    ff = wg.shape[1]
    sr = shared_out.shape[0]

    loads = [
        pltpu.make_async_copy(src, dst, w_sem.at[n])
        for n, (src, dst) in enumerate(
            [(sg_h, sg), (su_h, su), (sd_h, sd), (wg_h, wg), (wu_h, wu), (wd_h, wd)]
        )
    ]
    for load in loads:
        load.start()

    def ep_peer(step):
        return lax.rem(me + step, ep)

    def remote(src, dst, ssem, rsem, **where):
        copy = pltpu.make_async_remote_copy(
            src_ref=src, dst_ref=dst, send_sem=ssem, recv_sem=rsem,
            device_id=where, device_id_type=MESH,
        )
        copy.start()
        return copy

    barrier = pltpu.get_barrier_semaphore()
    for step in range(1, ep):
        pl.semaphore_signal(barrier, inc=1, device_id={"ep": ep_peer(step)}, device_id_type=MESH)
    for step in range(1, tp):
        pl.semaphore_signal(
            barrier, inc=1, device_id={"tp": lax.rem(j + step, tp)}, device_id_type=MESH
        )

    cols = pl.ds(pl.multiple_of(j * share, share), share)
    x_share = tokens[:, cols]
    c_share = cot[:, cols].astype(F32)
    slot_ids = lax.broadcasted_iota(jnp.int32, (rows, tok), 0)
    any_hot = jnp.zeros((rows, tok), F32)
    c_rows = jnp.zeros((rows, share), F32)
    for k in range(top):
        hot = jnp.where(slot_ids == slot_row[k : k + 1, :], 1.0, 0.0)
        any_hot = any_hot + hot
        c_rows = c_rows + dot(hot.astype(BF), (gates[:, k : k + 1] * c_share).astype(BF))
    x_rows = dot(any_hot.astype(BF), x_share)
    send[0] = x_rows.astype(BF).reshape(ep, cap_pad, share)
    send[1] = c_rows.astype(BF).reshape(ep, cap_pad, share)

    pl.semaphore_wait(barrier, ep + tp - 2)

    waits = []
    for step in range(1, ep):
        to = ep_peer(step)
        waits.append(
            remote(send.at[:, to], rx.at[j, :, me], d1_s.at[step], d1_r.at[step], ep=to)
        )
    rx[j, :, me] = send[:, me]

    def forward(source):
        block = rx.at[j, :, source]
        remote(block, block, d2_s.at[0], d2_r.at[j], tp=mate)
        for step in range(1, ny):
            to = lax.rem(y + step, ny) * CORES + core
            remote(block, block, d2_s.at[step], d2_r.at[j], tp=to)

    forward(me)

    for load in loads[:3]:
        load.wait()
    s_hidden, s_dg, s_du = activations(
        dot(tokens[...], sg[...]), dot(tokens[...], su[...]), dot(cot[...], sd[...], 1, 1)
    )

    d1 = list(waits)
    for step in range(1, ep):
        d1[step - 1].wait_recv()
        forward(lax.rem(me - step + ep, ep))

    for chunk in range(tp):
        at = slice(chunk * share, (chunk + 1) * share)
        value = dot(s_hidden, cot[:, at], 0, 0)
        for i in range(ep):
            term[i, :, at] = value[i * sr : (i + 1) * sr].astype(BF)
    for step in range(1, ep):
        to = ep_peer(step)
        waits.append(remote(term.at[to], term_rx.at[me], rs_s.at[step], rs_r.at[step], ep=to))
    rs = waits[ep - 1 :]

    def part_of(block, d_gate, d_up, gate_w, up_w):
        at = pl.ds(pl.multiple_of(block * share, share), share)
        return dot(d_gate, gate_w[at, :], 1, 1) + dot(d_up, up_w[at, :], 1, 1)

    for yq in range(ny):
        part_a[yq, rows:, :] = part_of(yq * CORES + 1 - core, s_dg, s_du, sg, su).astype(BF)
        part_own[yq, rows:, :] = part_of(yq * CORES + core, s_dg, s_du, sg, su)

    for load in loads[3:]:
        load.wait()
    acc[...] = jnp.zeros_like(acc)

    def add_share(t):
        at = pl.ds(pl.multiple_of(t * share, share), share)
        x_in = rx[t, 0].reshape(rows, share)
        c_in = rx[t, 1].reshape(rows, share)
        acc[0] += dot(x_in, wg[at, :])
        acc[1] += dot(x_in, wu[at, :])
        acc[2] += dot(c_in, wd[:, at], 1, 1)

    def arrived(t):
        pltpu.make_async_remote_copy(
            src_ref=rx.at[t], dst_ref=rx.at[t], send_sem=d2_s.at[0], recv_sem=d2_r.at[t],
            device_id={"tp": mate}, device_id_type=MESH,
        ).wait_recv()

    add_share(j)
    passed = []
    for step in range(1, ny):
        t = lax.rem(y - step + ny, ny) * CORES + core
        arrived(t)
        passed.append(remote(rx.at[t], rx.at[t], pass_s.at[step], d2_r.at[tp + step], tp=mate))
        if step == 1:
            arrived(mate)
            add_share(mate)
        add_share(t)
    for step in range(1, ny):
        t = lax.rem(y - step + ny, ny) * CORES + 1 - core
        passed[step - 1].wait_recv()
        add_share(t)

    outs = []
    for t in range(tp):
        at = pl.ds(t * share, share)
        outs.append(pltpu.make_async_copy(rx.at[t, 0], x_out.at[:, :, at], out_sem.at[2 * t]))
        outs.append(pltpu.make_async_copy(rx.at[t, 1], c_out.at[:, :, at], out_sem.at[2 * t + 1]))
    for out in outs:
        out.start()

    hidden, d_gate, d_up = activations(acc[0], acc[1], acc[2])
    hid_out[...] = hidden
    dg_out[...] = d_gate
    du_out[...] = d_up
    prod[...] = hidden.astype(F32) * acc[2]

    ra = []
    for yq in range(ny):
        part_a[yq, :rows, :] = part_of(yq * CORES + 1 - core, d_gate, d_up, wg, wu).astype(BF)
        ra.append(remote(part_a.at[yq], recv_a.at[yq], ra_s.at[yq], ra_r.at[yq], tp=mate))
    for yq in range(ny):
        part_own[yq, :rows, :] = part_of(yq * CORES + core, d_gate, d_up, wg, wu)

    gpart[...] = jnp.zeros_like(gpart)
    ones = jnp.ones((8, ff), F32)
    for i in range(ep):
        gpart[i, :, :cap_pad] = lax.dot_general(
            ones, prod[i * cap_pad : (i + 1) * cap_pad, :], (((1,), (1,)), ((), ())),
            preferred_element_type=F32, precision=lax.Precision.HIGHEST,
        )
    gx = []
    for step in range(1, tp):
        gx.append(remote(gpart, grecv.at[step], g_s.at[step], g_r.at[step], tp=lax.rem(j + step, tp)))

    for copy in ra:
        copy.wait_recv()
    rb = []
    for step in range(1, ny):
        yq = lax.rem(y + step, ny)
        part_b[step] = (part_own[yq] + recv_a[yq].astype(F32)).astype(BF)
        rb.append(
            remote(part_b.at[step], recv_b.at[step], rb_s.at[step], rb_r.at[step], tp=yq * CORES + core)
        )

    norm_down = jnp.zeros((ff, 1), F32)
    for t in range(tp):
        at = slice(t * share, (t + 1) * share)
        x_in = rx[t, 0].reshape(rows, share)
        c_in = rx[t, 1].reshape(rows, share)
        sq[0:1, at] = jnp.sum(jnp.square(dot(dg_out[...], x_in, 0, 0)), axis=0, keepdims=True)
        sq[1:2, at] = jnp.sum(jnp.square(dot(du_out[...], x_in, 0, 0)), axis=0, keepdims=True)
        norm_down += jnp.sum(jnp.square(dot(hid_out[...], c_in, 0, 0)), axis=1, keepdims=True)
    norm_down_out[...] = norm_down / width
    qx = []
    for step in range(1, tp):
        qx.append(remote(sq, sq_rx.at[step], q_s.at[step], q_r.at[step], tp=lax.rem(j + step, tp)))

    for copy in gx:
        copy.wait_recv()
    total = gpart[...]
    for step in range(1, tp):
        total = total + grecv[step]
    gsend[...] = total.astype(BF).astype(F32)
    gb = []
    for step in range(1, ep):
        to = ep_peer(step)
        gb.append(remote(gsend.at[to], gback.at[me], gb_s.at[step], gb_r.at[step], ep=to))
    gback[me] = gsend[me]

    for copy in rb:
        copy.wait_recv()
    part = part_own[y] + recv_a[y].astype(F32)
    for step in range(1, ny):
        part = part + recv_b[step].astype(F32)
    back_tx[...] = part[:rows].astype(BF).reshape(ep, cap_pad, share)
    shared_tot[...] = part[rows:]
    bk = []
    for step in range(1, ep):
        to = ep_peer(step)
        bk.append(remote(back_tx.at[to], back_rx.at[me], bk_s.at[step], bk_r.at[step], ep=to))
    back_rx[me] = back_tx[me]

    for copy in qx:
        copy.wait_recv()
    squares = sq[...]
    for step in range(1, tp):
        squares = squares + sq_rx[step]
    norm_in_out[...] = squares / (tp * ff)

    for copy in rs:
        copy.wait_recv()
    term_rx[me] = term[me]
    grad = term_rx[0].astype(F32)
    for i in range(1, ep):
        grad = grad + term_rx[i].astype(F32)
    shared_out[...] = grad
    norm_sh_out[...] = jnp.mean(jnp.square(grad), axis=1, keepdims=True)

    for copy in gb:
        copy.wait_recv()
    lane = lax.broadcasted_iota(jnp.int32, (tok, 128), 1)
    for k in range(top):
        picked = jnp.zeros((tok, 128), F32)
        for i in range(ep):
            hit = (lane < cap_pad) & (slot_col[:, k : k + 1] == lane + i * cap_pad)
            picked = picked + jnp.where(hit, gback[i, 0:1, :], 0.0)
        gate_out[:, k : k + 1] = jnp.sum(picked, axis=1, keepdims=True) / gates[:, k : k + 1]

    place = lax.broadcasted_iota(jnp.int32, (tok, rows), 1)
    pick = jnp.zeros((tok, rows), F32)
    for k in range(top):
        pick = pick + jnp.where(place == slot_col[:, k : k + 1], 1.0, 0.0)
    for copy in bk:
        copy.wait_recv()
    token_out[...] = (
        dot(pick.astype(BF), back_rx[...].reshape(rows, share)) + shared_tot[...]
    ).astype(BF)

    for step in range(ny):
        pltpu.make_async_remote_copy(
            src_ref=rx.at[j], dst_ref=rx.at[j], send_sem=d2_s.at[step], recv_sem=d2_r.at[j],
            device_id={"tp": mate}, device_id_type=MESH,
        ).wait_send()
    for copy in waits + passed + ra + gx + rb + qx + gb + bk:
        copy.wait_send()
    for out in outs:
        out.wait()


def on_device(
    ep, tp, tokens, routes, route_gates, cotangent, w_gate, w_up, w_down, s_gate, s_up, s_down
):
    tok, width = tokens.shape
    top = routes.shape[1]
    cap = max(2, (9 * tok * top + 8 * ep - 1) // (8 * ep))
    cap_pad = -(-cap // 16) * 16
    rows, share, ff, ny = ep * cap_pad, width // tp, w_gate.shape[2], tp // CORES
    sff = s_gate.shape[1]
    sr = sff // ep

    chosen = routes.reshape(tok * top)
    order = jnp.arange(tok * top, dtype=jnp.int32)
    earlier = (chosen[:, None] == chosen[None, :]) & (order[None, :] < order[:, None])
    slot = chosen * cap_pad + jnp.sum(earlier.astype(jnp.int32), axis=1)
    slot_col = slot.reshape(tok, top)

    vm, hbm = pl.BlockSpec(memory_space=pltpu.VMEM), pl.BlockSpec(memory_space=pl.ANY)
    dma, sds = pltpu.SemaphoreType.DMA, jax.ShapeDtypeStruct
    out_shape = [
        sds((tok, share), BF), sds((tok, top), F32), sds((sr, width), F32), sds((2, width), F32),
        sds((ff, 1), F32), sds((sr, 1), F32),
        sds((ep, cap_pad, width), BF), sds((ep, cap_pad, width), BF),
        sds((rows, ff), BF), sds((rows, ff), BF), sds((rows, ff), BF),
    ]
    joint = rows + tok
    scratch = [
        pltpu.VMEM((width, ff), BF), pltpu.VMEM((width, ff), BF), pltpu.VMEM((ff, width), BF),
        pltpu.VMEM((width, sff), BF), pltpu.VMEM((width, sff), BF), pltpu.VMEM((sff, width), BF),
        pltpu.VMEM((2, ep, cap_pad, share), BF),
        pltpu.VMEM((tp, 2, ep, cap_pad, share), BF),
        pltpu.VMEM((3, rows, ff), F32), pltpu.VMEM((rows, ff), F32),
        pltpu.VMEM((ep, sr, width), BF), pltpu.VMEM((ep, sr, width), BF),
        pltpu.VMEM((ny, joint, share), BF), pltpu.VMEM((ny, joint, share), F32),
        pltpu.VMEM((ny, joint, share), BF), pltpu.VMEM((ny, joint, share), BF),
        pltpu.VMEM((ny, joint, share), BF),
        pltpu.VMEM((ep, cap_pad, share), BF), pltpu.VMEM((ep, cap_pad, share), BF),
        pltpu.VMEM((tok, share), F32),
        pltpu.VMEM((ep, 8, 128), F32), pltpu.VMEM((tp, ep, 8, 128), F32),
        pltpu.VMEM((ep, 8, 128), F32), pltpu.VMEM((ep, 8, 128), F32),
        pltpu.VMEM((2, width), F32), pltpu.VMEM((tp, 2, width), F32),
        dma((6,)), dma((2 * tp,)), dma((ep,)), dma((ep,)), dma((ny,)), dma((tp + ny,)), dma((ny,)),
        dma((ep,)), dma((ep,)), dma((ny,)), dma((ny,)), dma((ny,)), dma((ny,)),
        dma((ep,)), dma((ep,)), dma((tp,)), dma((tp,)), dma((ep,)), dma((ep,)), dma((tp,)), dma((tp,)),
    ]
    out = pl.pallas_call(
        functools.partial(body, ep, tp, cap_pad),
        out_shape=out_shape,
        in_specs=[vm] * 5 + [hbm] * 6,
        out_specs=[vm] * 6 + [hbm] * 2 + [vm] * 3,
        scratch_shapes=scratch,
        compiler_params=pltpu.CompilerParams(
            collective_id=0, has_side_effects=True, vmem_limit_bytes=60 * 1024 * 1024
        ),
    )(
        slot_col.T, slot_col, route_gates, tokens, cotangent,
        w_gate[0], w_up[0], w_down[0], s_gate, s_up, s_down,
    )
    token_grad, gate_grad, grad_shared, norm_in, norm_down, norm_sh, x, c, hid, dg, du = out
    x, c = x.reshape(rows, width), c.reshape(rows, width)
    return (
        token_grad, gate_grad, dot(x, dg, 0, 0)[None], dot(x, du, 0, 0)[None],
        dot(hid, c, 0, 0)[None], grad_shared, norm_in[None], norm_down.reshape(1, ff),
        norm_sh.reshape(sr),
    )


def solution(mesh):
    placed = (
        P("ep", None), P("ep", None), P("ep", None), P("ep", None),
        P("ep", None, "tp"), P("ep", None, "tp"), P("ep", "tp", None),
        P(None, "tp"), P(None, "tp"), P("tp", None),
    )
    return jax.shard_map(
        functools.partial(on_device, mesh.shape["ep"], mesh.shape["tp"]),
        mesh=mesh,
        in_specs=placed,
        out_specs=(
            P("ep", "tp"), P("ep", None), P("ep", None, "tp"), P("ep", None, "tp"),
            P("ep", "tp", None), P(("tp", "ep"), None), P("ep", None, None), P("ep", "tp"),
            P(("tp", "ep")),
        ),
        check_vma=False,
    )
```

```python
import functools

import jax
import jax.numpy as jnp
from jax import lax
from jax.experimental import pallas as pl
from jax.experimental.pallas import tpu as pltpu
from jax.sharding import PartitionSpec as P

MESH = pl.DeviceIdType.MESH
CORES = 2
BF = jnp.bfloat16
F32 = jnp.float32


def dot(a, b, ca=1, cb=0):
    return lax.dot_general(a, b, (((ca,), (cb,)), ((), ())), preferred_element_type=F32)


def activations(pre_gate, pre_up, hidden_grad):
    sig = jax.nn.sigmoid(pre_gate)
    act = pre_gate * sig
    hidden = (act * pre_up).astype(BF)
    d_gate = (hidden_grad * pre_up * sig * (1.0 + pre_gate * (1.0 - sig))).astype(BF)
    d_up = (hidden_grad * act).astype(BF)
    return hidden, d_gate, d_up


def body(
    ep, tp, cap_pad, live,
    routes, gate_rows, tokens, cot, wg_h, wu_h, wd_h, sg_h, su_h, sd_h,
    token_out, gate_out, shared_out, norm_in_out, norm_down_out, norm_sh_out,
    x_out, c_out, hid_out, dg_out, du_out,
    wg, wu, wd, sg, su, sd, send, rx, acc, prod, term, term_rx, pair, pair_rx,
    part_a, part_own, recv_a, part_b, recv_b, sh_a, sh_own, sh_recv_a, sh_b, sh_recv_b,
    back_tx, back_rx, gpart, grecv, gsend, gback, sq, sq_rx,
    w_sem, out_sem, d1_s, d1_r, d2_s, d2_r, pass_s, rs_s, rs_r, rp_s, rp_r, ra_s, ra_r, rb_s, rb_r,
    bk_s, bk_r, g_s, g_r, gb_s, gb_r, q_s, q_r, sa_s, sa_r, sb_s, sb_r,
):
    me = lax.axis_index("ep")
    j = lax.axis_index("tp")
    core = lax.rem(j, CORES)
    y = lax.div(j, CORES)
    mate = j + 1 - 2 * core
    ny = tp // CORES
    rows = ep * cap_pad
    tok, width = tokens.shape
    share = width // tp
    top = routes.shape[0]
    px = lax.rem(me, 2)
    group = lax.div(me, 2)
    groups = ep // 2
    ff = wg.shape[1]
    sr = shared_out.shape[0]

    loads = [
        pltpu.make_async_copy(src, dst, w_sem.at[n])
        for n, (src, dst) in enumerate(
            [(sg_h, sg), (su_h, su), (sd_h, sd), (wg_h, wg), (wu_h, wu), (wd_h, wd)]
        )
    ]
    for load in loads:
        load.start()

    def ep_peer(step):
        return lax.rem(me + step, ep)

    def remote(src, dst, ssem, rsem, **where):
        copy = pltpu.make_async_remote_copy(
            src_ref=src, dst_ref=dst, send_sem=ssem, recv_sem=rsem,
            device_id=where, device_id_type=MESH,
        )
        copy.start()
        return copy

    barrier = pltpu.get_barrier_semaphore()
    for step in range(1, ep):
        pl.semaphore_signal(barrier, inc=1, device_id={"ep": ep_peer(step)}, device_id_type=MESH)
    for step in range(1, tp):
        pl.semaphore_signal(
            barrier, inc=1, device_id={"tp": lax.rem(j + step, tp)}, device_id_type=MESH
        )

    if live < cap_pad:
        rx[:, :, :, live:, :] = jnp.zeros((tp, 2, ep, cap_pad - live, share), BF)
        back_rx[:, live:, :] = jnp.zeros((ep, cap_pad - live, share), BF)

    sub = lax.broadcasted_iota(jnp.int32, (tok, tok), 0)
    lane = lax.broadcasted_iota(jnp.int32, (tok, tok), 1)

    def to_col(row):
        return jnp.sum(jnp.where(sub == lane, row, 0.0), axis=1, keepdims=True)

    def to_row(col):
        return jnp.sum(jnp.where(sub == lane, col, 0.0), axis=0, keepdims=True)

    expert_row = [routes[k : k + 1, :].astype(F32) for k in range(top)]
    expert_col = [to_col(row) for row in expert_row]
    gate_col = [to_col(gate_rows[k : k + 1, :]) for k in range(top)]
    slot_row = []
    for k in range(top):
        slot = expert_row[k] * cap_pad
        for other in range(top):
            same = (expert_col[other] == expert_row[k]) & (sub < lane)
            slot = slot + jnp.sum(jnp.where(same, 1.0, 0.0), axis=0, keepdims=True)
        slot_row.append(slot)
    slot_col = [to_col(row) for row in slot_row]

    cols = pl.ds(pl.multiple_of(j * share, share), share)
    x_share = tokens[:, cols]
    c_share = cot[:, cols].astype(F32)
    slot_ids = lax.broadcasted_iota(jnp.int32, (rows, tok), 0).astype(F32)
    any_hot = jnp.zeros((rows, tok), F32)
    c_rows = jnp.zeros((rows, share), F32)
    for k in range(top):
        hot = jnp.where(slot_ids == slot_row[k], 1.0, 0.0)
        any_hot = any_hot + hot
        c_rows = c_rows + dot(hot.astype(BF), (gate_col[k] * c_share).astype(BF))
    x_rows = dot(any_hot.astype(BF), x_share)
    send[0] = x_rows.astype(BF).reshape(ep, cap_pad, share)
    send[1] = c_rows.astype(BF).reshape(ep, cap_pad, share)

    pl.semaphore_wait(barrier, ep + tp - 2)

    filled = pl.ds(0, live)
    far_first = sorted(range(1, ep), key=lambda step: -min(step, ep - step))
    waits, d1 = [], {}
    for step in far_first:
        to = ep_peer(step)
        d1[step] = remote(
            send.at[:, to, filled], rx.at[j, :, me, filled], d1_s.at[step], d1_r.at[step], ep=to
        )
        waits.append(d1[step])
    rx[j, :, me] = send[:, me]

    def forward(source):
        block = rx.at[j, :, source, filled]
        remote(block, block, d2_s.at[0], d2_r.at[j], tp=mate)
        for step in range(1, ny):
            to = lax.rem(y + step, ny) * CORES + core
            remote(block, block, d2_s.at[step], d2_r.at[j], tp=to)

    forward(me)

    def part_of(block, d_gate, d_up, gate_w, up_w):
        at = pl.ds(pl.multiple_of(block * share, share), share)
        return dot(d_gate, gate_w[at, :], 1, 1) + dot(d_up, up_w[at, :], 1, 1)

    far_y = [lax.rem(y + step, ny) for step in range(1, ny)] + [y]

    held, sa, rs = {}, [], []

    def shared_gate():
        loads[0].wait()
        held["gate"] = dot(tokens[...], sg[...])

    def shared_up():
        loads[1].wait()
        held["up"] = dot(tokens[...], su[...])

    def shared_act():
        loads[2].wait()
        held["act"] = activations(held["gate"], held["up"], dot(cot[...], sd[...], 1, 1))

    def shared_term(chunks):
        for chunk in chunks:
            at = slice(chunk * share, (chunk + 1) * share)
            value = dot(held["act"][0], cot[:, at], 0, 0)
            for i in range(ep):
                term[i % 2, i // 2, :, at] = value[i * sr : (i + 1) * sr].astype(BF)

    def shared_send():
        for d in range(groups):
            rs.append(
                remote(
                    term.at[1 - px, d], term_rx.at[d], rs_s.at[d], rs_r.at[d],
                    ep=me + 1 - 2 * px,
                )
            )

    def shared_parts():
        for n, yq in enumerate(far_y):
            sh_a[n] = part_of(yq * CORES + 1 - core, *held["act"][1:], sg, su).astype(BF)
            sa.append(remote(sh_a.at[n], sh_recv_a.at[n], sa_s.at[n], sa_r.at[n], tp=mate))

    def shared_own():
        for n, yq in enumerate(far_y):
            sh_own[n] = part_of(yq * CORES + core, *held["act"][1:], sg, su)

    tasks = [
        shared_gate, shared_up, shared_act, lambda: shared_term(range(tp // 2)),
        lambda: (shared_term(range(tp // 2, tp)), shared_send()), shared_parts, shared_own,
    ]
    stride = -(-(ep - 1) // len(tasks))
    for n, task in enumerate(tasks):
        task()
        for step in far_first[n * stride : (n + 1) * stride]:
            d1[step].wait_recv()
            forward(lax.rem(me - step + ep, ep))

    for load in loads[3:]:
        load.wait()
    acc[...] = jnp.zeros_like(acc)

    def add_share(t):
        at = pl.ds(pl.multiple_of(t * share, share), share)
        x_in = rx[t, 0].reshape(rows, share)
        c_in = rx[t, 1].reshape(rows, share)
        acc[0] += dot(x_in, wg[at, :])
        acc[1] += dot(x_in, wu[at, :])
        acc[2] += dot(c_in, wd[:, at], 1, 1)

    def arrived(t):
        pltpu.make_async_remote_copy(
            src_ref=rx.at[t, :, :, filled], dst_ref=rx.at[t, :, :, filled],
            send_sem=d2_s.at[0], recv_sem=d2_r.at[t],
            device_id={"tp": mate}, device_id_type=MESH,
        ).wait_recv()

    add_share(j)
    passed = []
    for step in range(1, ny):
        t = lax.rem(y - step + ny, ny) * CORES + core
        arrived(t)
        whole = rx.at[t, :, :, filled]
        passed.append(remote(whole, whole, pass_s.at[step], d2_r.at[tp + step], tp=mate))
        if step == 1:
            arrived(mate)
            add_share(mate)
        add_share(t)
    for step in range(1, ny):
        t = lax.rem(y - step + ny, ny) * CORES + 1 - core
        passed[step - 1].wait_recv()
        add_share(t)

    sb = []
    for n, yq in enumerate(far_y[:-1]):
        sa[n].wait_recv()
        sh_b[n] = (sh_own[n] + sh_recv_a[n].astype(F32)).astype(BF)
        sb.append(
            remote(sh_b.at[n], sh_recv_b.at[n], sb_s.at[n], sb_r.at[n], tp=yq * CORES + core)
        )

    outs = []
    for t in range(tp):
        at = pl.ds(t * share, share)
        outs.append(pltpu.make_async_copy(rx.at[t, 0], x_out.at[:, :, at], out_sem.at[2 * t]))
        outs.append(pltpu.make_async_copy(rx.at[t, 1], c_out.at[:, :, at], out_sem.at[2 * t + 1]))
    for out in outs:
        out.start()

    hidden, d_gate, d_up = activations(acc[0], acc[1], acc[2])
    hid_out[...] = hidden
    dg_out[...] = d_gate
    du_out[...] = d_up
    prod[...] = hidden.astype(F32) * acc[2]

    ra = []
    for n, yq in enumerate(far_y):
        value = part_of(yq * CORES + 1 - core, d_gate, d_up, wg, wu).astype(BF)
        part_a[n] = value.reshape(ep, cap_pad, share)
        ra.append(
            remote(part_a.at[n, :, filled], recv_a.at[n, :, filled], ra_s.at[n], ra_r.at[n], tp=mate)
        )
    rb = []
    for n, yq in enumerate(far_y):
        value = part_of(yq * CORES + core, d_gate, d_up, wg, wu)
        part_own[n] = value.reshape(ep, cap_pad, share)
        if n < ny - 1:
            ra[n].wait_recv()
            part_b[n] = (part_own[n] + recv_a[n].astype(F32)).astype(BF)
            rb.append(
                remote(
                    part_b.at[n, :, filled], recv_b.at[n, :, filled], rb_s.at[n], rb_r.at[n],
                    tp=yq * CORES + core,
                )
            )

    rp = []
    for d in range(groups):
        rs[d].wait_recv()
    for step in range(groups):
        d = lax.rem(group + step, groups)
        pair[d] = (term[px, d].astype(F32) + term_rx[d].astype(F32)).astype(BF)
        if step > 0:
            rp.append(
                remote(
                    pair.at[d], pair_rx.at[group], rp_s.at[step], rp_r.at[step], ep=2 * d + px
                )
            )
    pair_rx[group] = pair[group]

    gpart[...] = jnp.zeros_like(gpart)
    ones = jnp.ones((8, ff), F32)
    for i in range(ep):
        gpart[i, :, :cap_pad] = lax.dot_general(
            ones, prod[i * cap_pad : (i + 1) * cap_pad, :], (((1,), (1,)), ((), ())),
            preferred_element_type=F32, precision=lax.Precision.HIGHEST,
        )
    gx = []
    for step in range(1, tp):
        gx.append(remote(gpart, grecv.at[step], g_s.at[step], g_r.at[step], tp=lax.rem(j + step, tp)))

    for copy in gx:
        copy.wait_recv()
    total = gpart[...]
    for step in range(1, tp):
        total = total + grecv[step]
    gsend[...] = total.astype(BF).astype(F32)
    gb = []
    for step in range(1, ep):
        to = ep_peer(step)
        gb.append(remote(gsend.at[to], gback.at[me], gb_s.at[step], gb_r.at[step], ep=to))
    gback[me] = gsend[me]

    ra[ny - 1].wait_recv()
    part = part_own[ny - 1] + recv_a[ny - 1].astype(F32)
    for n in range(ny - 1):
        rb[n].wait_recv()
        part = part + recv_b[n].astype(F32)
    back_tx[...] = part.astype(BF)
    bk = []
    for step in range(1, ep):
        to = ep_peer(step)
        bk.append(
            remote(
                back_tx.at[to, filled], back_rx.at[me, filled], bk_s.at[step], bk_r.at[step], ep=to
            )
        )
    back_rx[me, :live] = back_tx[me, :live]

    sa[ny - 1].wait_recv()
    shared_tot = sh_own[ny - 1] + sh_recv_a[ny - 1].astype(F32)
    for n in range(ny - 1):
        sb[n].wait_recv()
        shared_tot = shared_tot + sh_recv_b[n].astype(F32)

    norm_down = jnp.zeros((1, ff), F32)
    for t in range(tp):
        at = slice(t * share, (t + 1) * share)
        x_in = rx[t, 0].reshape(rows, share)
        c_in = rx[t, 1].reshape(rows, share)
        sq[0:1, at] = jnp.sum(jnp.square(dot(dg_out[...], x_in, 0, 0)), axis=0, keepdims=True)
        sq[1:2, at] = jnp.sum(jnp.square(dot(du_out[...], x_in, 0, 0)), axis=0, keepdims=True)
        norm_down += jnp.sum(jnp.square(dot(c_in, hid_out[...], 0, 0)), axis=0, keepdims=True)
    norm_down_out[...] = norm_down / width
    qx = []
    for step in range(1, tp):
        qx.append(remote(sq, sq_rx.at[step], q_s.at[step], q_r.at[step], tp=lax.rem(j + step, tp)))

    for copy in qx:
        copy.wait_recv()
    squares = sq[...]
    for step in range(1, tp):
        squares = squares + sq_rx[step]
    norm_in_out[...] = squares / (tp * ff)

    for copy in rp:
        copy.wait_recv()
    grad = pair_rx[0].astype(F32)
    for i in range(1, groups):
        grad = grad + pair_rx[i].astype(F32)
    shared_out[...] = grad
    norm_sh = jnp.mean(jnp.square(grad), axis=1, keepdims=True)
    here = lax.broadcasted_iota(jnp.int32, (sr, sr), 0) == lax.broadcasted_iota(
        jnp.int32, (sr, sr), 1
    )
    norm_sh_out[...] = jnp.sum(jnp.where(here, norm_sh, 0.0), axis=0, keepdims=True)

    for copy in gb:
        copy.wait_recv()
    spot = lax.broadcasted_iota(jnp.int32, (tok, 128), 1)
    spot_f = spot.astype(F32)
    for k in range(top):
        picked = jnp.zeros((tok, 128), F32)
        for i in range(ep):
            hit = (spot < cap_pad) & (slot_col[k] == spot_f + float(i * cap_pad))
            picked = picked + jnp.where(hit, gback[i, 0:1, :], 0.0)
        dots = to_row(jnp.sum(picked, axis=1, keepdims=True))
        gate_out[k : k + 1, :] = dots / gate_rows[k : k + 1, :]

    place = lax.broadcasted_iota(jnp.int32, (tok, rows), 1).astype(F32)
    pick = jnp.zeros((tok, rows), F32)
    for k in range(top):
        pick = pick + jnp.where(place == slot_col[k], 1.0, 0.0)
    for copy in bk:
        copy.wait_recv()
    token_out[...] = (
        dot(pick.astype(BF), back_rx[...].reshape(rows, share)) + shared_tot
    ).astype(BF)

    sent = rx.at[j, :, :, filled]
    for step in range(ny):
        pltpu.make_async_remote_copy(
            src_ref=sent, dst_ref=sent, send_sem=d2_s.at[step], recv_sem=d2_r.at[j],
            device_id={"tp": mate}, device_id_type=MESH,
        ).wait_send()
    for copy in waits + passed + ra + gx + rb + qx + gb + bk + rs + rp + sa + sb:
        copy.wait_send()
    for out in outs:
        out.wait()


def on_device(
    ep, tp, tokens, routes, route_gates, cotangent, w_gate, w_up, w_down, s_gate, s_up, s_down
):
    tok, width = tokens.shape
    top = routes.shape[1]
    cap = max(2, (9 * tok * top + 8 * ep - 1) // (8 * ep))
    cap_pad = -(-cap // 16) * 16
    rows, share, ff, ny = ep * cap_pad, width // tp, w_gate.shape[2], tp // CORES
    sff = s_gate.shape[1]
    sr = sff // ep

    live = -(-cap // 8) * 8

    vm, hbm = pl.BlockSpec(memory_space=pltpu.VMEM), pl.BlockSpec(memory_space=pl.ANY)
    dma, sds = pltpu.SemaphoreType.DMA, jax.ShapeDtypeStruct
    out_shape = [
        sds((tok, share), BF), sds((top, tok), F32), sds((sr, width), F32), sds((2, width), F32),
        sds((1, ff), F32), sds((1, sr), F32),
        sds((ep, cap_pad, width), BF), sds((ep, cap_pad, width), BF),
        sds((rows, ff), BF), sds((rows, ff), BF), sds((rows, ff), BF),
    ]
    slots = (ny, ep, cap_pad, share)
    scratch = [
        pltpu.VMEM((width, ff), BF), pltpu.VMEM((width, ff), BF), pltpu.VMEM((ff, width), BF),
        pltpu.VMEM((width, sff), BF), pltpu.VMEM((width, sff), BF), pltpu.VMEM((sff, width), BF),
        pltpu.VMEM((2, ep, cap_pad, share), BF),
        pltpu.VMEM((tp, 2, ep, cap_pad, share), BF),
        pltpu.VMEM((3, rows, ff), F32), pltpu.VMEM((rows, ff), F32),
        pltpu.VMEM((2, ep // 2, sr, width), BF), pltpu.VMEM((ep // 2, sr, width), BF),
        pltpu.VMEM((ep // 2, sr, width), BF), pltpu.VMEM((ep // 2, sr, width), BF),
        pltpu.VMEM(slots, BF), pltpu.VMEM(slots, F32), pltpu.VMEM(slots, BF),
        pltpu.VMEM(slots, BF), pltpu.VMEM(slots, BF),
        pltpu.VMEM((ny, tok, share), BF), pltpu.VMEM((ny, tok, share), F32),
        pltpu.VMEM((ny, tok, share), BF), pltpu.VMEM((ny, tok, share), BF),
        pltpu.VMEM((ny, tok, share), BF),
        pltpu.VMEM((ep, cap_pad, share), BF), pltpu.VMEM((ep, cap_pad, share), BF),
        pltpu.VMEM((ep, 8, 128), F32), pltpu.VMEM((tp, ep, 8, 128), F32),
        pltpu.VMEM((ep, 8, 128), F32), pltpu.VMEM((ep, 8, 128), F32),
        pltpu.VMEM((2, width), F32), pltpu.VMEM((tp, 2, width), F32),
        dma((6,)), dma((2 * tp,)), dma((ep,)), dma((ep,)), dma((ny,)), dma((tp + ny,)), dma((ny,)),
        dma((ep,)), dma((ep,)), dma((ep,)), dma((ep,)), dma((ny,)), dma((ny,)), dma((ny,)), dma((ny,)),
        dma((ep,)), dma((ep,)), dma((tp,)), dma((tp,)), dma((ep,)), dma((ep,)), dma((tp,)), dma((tp,)),
        dma((ny,)), dma((ny,)), dma((ny,)), dma((ny,)),
    ]
    out = pl.pallas_call(
        functools.partial(body, ep, tp, cap_pad, live),
        out_shape=out_shape,
        in_specs=[vm] * 4 + [hbm] * 6,
        out_specs=[vm] * 6 + [hbm] * 2 + [vm] * 3,
        scratch_shapes=scratch,
        compiler_params=pltpu.CompilerParams(
            collective_id=0, has_side_effects=True, vmem_limit_bytes=60 * 1024 * 1024
        ),
    )(
        routes.T, route_gates.T, tokens, cotangent,
        w_gate[0], w_up[0], w_down[0], s_gate, s_up, s_down,
    )
    token_grad, gate_grad, grad_shared, norm_in, norm_down, norm_sh, x, c, hid, dg, du = out
    x, c = x.reshape(rows, width), c.reshape(rows, width)
    return (
        token_grad, gate_grad.T, dot(x, dg, 0, 0)[None], dot(x, du, 0, 0)[None],
        dot(hid, c, 0, 0)[None], grad_shared, norm_in[None], norm_down.reshape(1, ff),
        norm_sh.reshape(sr),
    )


def solution(mesh):
    placed = (
        P("ep", None), P("ep", None), P("ep", None), P("ep", None),
        P("ep", None, "tp"), P("ep", None, "tp"), P("ep", "tp", None),
        P(None, "tp"), P(None, "tp"), P("tp", None),
    )
    return jax.shard_map(
        functools.partial(on_device, mesh.shape["ep"], mesh.shape["tp"]),
        mesh=mesh,
        in_specs=placed,
        out_specs=(
            P("ep", "tp"), P("ep", None), P("ep", None, "tp"), P("ep", None, "tp"),
            P("ep", "tp", None), P(("tp", "ep"), None), P("ep", None, None), P("ep", "tp"),
            P(("tp", "ep")),
        ),
        check_vma=False,
    )
```

```python
import functools

import jax
import jax.numpy as jnp
from jax import lax
from jax.experimental import pallas as pl
from jax.experimental.pallas import tpu as pltpu
from jax.sharding import PartitionSpec as P

MESH = pl.DeviceIdType.MESH
CORES = 2
BF = jnp.bfloat16
F32 = jnp.float32


def dot(a, b, ca=1, cb=0):
    return lax.dot_general(a, b, (((ca,), (cb,)), ((), ())), preferred_element_type=F32)


def activations(pre_gate, pre_up, hidden_grad):
    sig = jax.nn.sigmoid(pre_gate)
    act = pre_gate * sig
    hidden = (act * pre_up).astype(BF)
    d_gate = (hidden_grad * pre_up * sig * (1.0 + pre_gate * (1.0 - sig))).astype(BF)
    d_up = (hidden_grad * act).astype(BF)
    return hidden, d_gate, d_up


def body(
    ep, tp, cap_pad, live,
    routes, gate_rows, tokens, cot, wg_h, wu_h, wd_h, sg_h, su_h, sd_h,
    token_out, gate_out, shared_out, norm_in_out, norm_down_out, norm_sh_out,
    x_out, c_out, hid_out, dg_out, du_out,
    wg, wu, wd, sg, su, sd, send, rx, acc, prod, term, term_rx, pair, pair_rx,
    part_a, part_own, recv_a, part_b, recv_b, sh_a, sh_own, sh_recv_a, sh_b, sh_recv_b,
    back_tx, back_rx, gpart, grecv, gsend, gback, sq, sq_rx,
    w_sem, out_sem, d1_s, d1_r, d2_s, d2_r, pass_s, rs_s, rs_r, rp_s, rp_r, ra_s, ra_r, rb_s, rb_r,
    bk_s, bk_r, g_s, g_r, gb_s, gb_r, q_s, q_r, sa_s, sa_r, sb_s, sb_r,
):
    me = lax.axis_index("ep")
    j = lax.axis_index("tp")
    core = lax.rem(j, CORES)
    y = lax.div(j, CORES)
    mate = j + 1 - 2 * core
    ny = tp // CORES
    rows = ep * cap_pad
    tok, width = tokens.shape
    share = width // tp
    top = routes.shape[0]
    px = lax.rem(me, 2)
    group = lax.div(me, 2)
    groups = ep // 2
    ff = wg.shape[1]
    sr = shared_out.shape[0]

    loads = [
        pltpu.make_async_copy(src, dst, w_sem.at[n])
        for n, (src, dst) in enumerate(
            [(sg_h, sg), (su_h, su), (sd_h, sd), (wg_h, wg), (wu_h, wu), (wd_h, wd)]
        )
    ]
    for load in loads:
        load.start()

    def ep_peer(step):
        return lax.rem(me + step, ep)

    def remote(src, dst, ssem, rsem, **where):
        copy = pltpu.make_async_remote_copy(
            src_ref=src, dst_ref=dst, send_sem=ssem, recv_sem=rsem,
            device_id=where, device_id_type=MESH,
        )
        copy.start()
        return copy

    barrier = pltpu.get_barrier_semaphore()
    for step in range(1, ep):
        pl.semaphore_signal(barrier, inc=1, device_id={"ep": ep_peer(step)}, device_id_type=MESH)
    for step in range(1, tp):
        pl.semaphore_signal(
            barrier, inc=1, device_id={"tp": lax.rem(j + step, tp)}, device_id_type=MESH
        )

    if live < cap_pad:
        rx[:, :, :, live:, :] = jnp.zeros((tp, 2, ep, cap_pad - live, share), BF)
        back_rx[:, live:, :] = jnp.zeros((ep, cap_pad - live, share), BF)

    sub = lax.broadcasted_iota(jnp.int32, (tok, tok), 0)
    lane = lax.broadcasted_iota(jnp.int32, (tok, tok), 1)

    def to_col(row):
        return jnp.sum(jnp.where(sub == lane, row, 0.0), axis=1, keepdims=True)

    def to_row(col):
        return jnp.sum(jnp.where(sub == lane, col, 0.0), axis=0, keepdims=True)

    expert_row = [routes[k : k + 1, :].astype(F32) for k in range(top)]
    expert_col = [to_col(row) for row in expert_row]
    gate_col = [to_col(gate_rows[k : k + 1, :]) for k in range(top)]
    slot_row = []
    for k in range(top):
        slot = expert_row[k] * cap_pad
        for other in range(top):
            same = (expert_col[other] == expert_row[k]) & (sub < lane)
            slot = slot + jnp.sum(jnp.where(same, 1.0, 0.0), axis=0, keepdims=True)
        slot_row.append(slot)
    slot_col = [to_col(row) for row in slot_row]

    cols = pl.ds(pl.multiple_of(j * share, share), share)
    x_share = tokens[:, cols]
    c_share = cot[:, cols].astype(F32)
    slot_ids = lax.broadcasted_iota(jnp.int32, (rows, tok), 0).astype(F32)
    any_hot = jnp.zeros((rows, tok), F32)
    c_rows = jnp.zeros((rows, share), F32)
    for k in range(top):
        hot = jnp.where(slot_ids == slot_row[k], 1.0, 0.0)
        any_hot = any_hot + hot
        c_rows = c_rows + dot(hot.astype(BF), (gate_col[k] * c_share).astype(BF))
    x_rows = dot(any_hot.astype(BF), x_share)
    send[0] = x_rows.astype(BF).reshape(ep, cap_pad, share)
    send[1] = c_rows.astype(BF).reshape(ep, cap_pad, share)

    pl.semaphore_wait(barrier, ep + tp - 2)

    filled = pl.ds(0, live)
    far_first = sorted(range(1, ep), key=lambda step: -min(step, ep - step))
    waits, d1 = [], {}
    for step in far_first:
        to = ep_peer(step)
        d1[step] = remote(
            send.at[:, to, filled], rx.at[j, :, me, filled], d1_s.at[step], d1_r.at[step], ep=to
        )
        waits.append(d1[step])
    rx[j, :, me] = send[:, me]

    def forward(source):
        block = rx.at[j, :, source, filled]
        remote(block, block, d2_s.at[0], d2_r.at[j], tp=mate)
        for step in range(1, ny):
            to = lax.rem(y + step, ny) * CORES + core
            remote(block, block, d2_s.at[step], d2_r.at[j], tp=to)

    forward(me)

    def part_of(block, d_gate, d_up, gate_w, up_w):
        at = pl.ds(pl.multiple_of(block * share, share), share)
        return dot(d_gate, gate_w[at, :], 1, 1) + dot(d_up, up_w[at, :], 1, 1)

    far_y = [lax.rem(y + step, ny) for step in range(1, ny)] + [y]

    held, sa, rs = {}, [], []

    def shared_gate():
        loads[0].wait()
        held["gate"] = dot(tokens[...], sg[...])

    def shared_up():
        loads[1].wait()
        held["up"] = dot(tokens[...], su[...])

    def shared_act():
        loads[2].wait()
        held["act"] = activations(held["gate"], held["up"], dot(cot[...], sd[...], 1, 1))

    def shared_term(chunks):
        for chunk in chunks:
            at = slice(chunk * share, (chunk + 1) * share)
            value = dot(held["act"][0], cot[:, at], 0, 0)
            for i in range(ep):
                term[i % 2, i // 2, :, at] = value[i * sr : (i + 1) * sr].astype(BF)

    def shared_send():
        for d in range(groups):
            rs.append(
                remote(
                    term.at[1 - px, d], term_rx.at[d], rs_s.at[d], rs_r.at[d],
                    ep=me + 1 - 2 * px,
                )
            )

    def shared_parts():
        for n, yq in enumerate(far_y):
            sh_a[n] = part_of(yq * CORES + 1 - core, *held["act"][1:], sg, su).astype(BF)
            sa.append(remote(sh_a.at[n], sh_recv_a.at[n], sa_s.at[n], sa_r.at[n], tp=mate))

    def shared_own():
        for n, yq in enumerate(far_y):
            sh_own[n] = part_of(yq * CORES + core, *held["act"][1:], sg, su)

    tasks = [
        shared_gate, shared_up, shared_act, lambda: shared_term(range(tp // 2)),
        lambda: (shared_term(range(tp // 2, tp)), shared_send()), shared_parts, shared_own,
    ]
    stride = -(-(ep - 1) // len(tasks))
    for n, task in enumerate(tasks):
        task()
        for step in far_first[n * stride : (n + 1) * stride]:
            d1[step].wait_recv()
            forward(lax.rem(me - step + ep, ep))

    for load in loads[3:]:
        load.wait()
    acc[...] = jnp.zeros_like(acc)

    def add_share(t):
        at = pl.ds(pl.multiple_of(t * share, share), share)
        x_in = rx[t, 0].reshape(rows, share)
        c_in = rx[t, 1].reshape(rows, share)
        acc[0] += dot(x_in, wg[at, :])
        acc[1] += dot(x_in, wu[at, :])
        acc[2] += dot(c_in, wd[:, at], 1, 1)

    def arrived(t):
        pltpu.make_async_remote_copy(
            src_ref=rx.at[t, :, :, filled], dst_ref=rx.at[t, :, :, filled],
            send_sem=d2_s.at[0], recv_sem=d2_r.at[t],
            device_id={"tp": mate}, device_id_type=MESH,
        ).wait_recv()

    add_share(j)
    passed = []
    for step in range(1, ny):
        t = lax.rem(y - step + ny, ny) * CORES + core
        arrived(t)
        whole = rx.at[t, :, :, filled]
        passed.append(remote(whole, whole, pass_s.at[step], d2_r.at[tp + step], tp=mate))
        if step == 1:
            arrived(mate)
            add_share(mate)
        add_share(t)
    for step in range(1, ny):
        t = lax.rem(y - step + ny, ny) * CORES + 1 - core
        passed[step - 1].wait_recv()
        add_share(t)

    rp = []
    for d in range(groups):
        rs[d].wait_recv()
    for step in range(groups):
        d = lax.rem(group + step, groups)
        pair[d] = (term[px, d].astype(F32) + term_rx[d].astype(F32)).astype(BF)
        if step > 0:
            rp.append(
                remote(
                    pair.at[d], pair_rx.at[group], rp_s.at[step], rp_r.at[step], ep=2 * d + px
                )
            )
    pair_rx[group] = pair[group]

    sb = []
    for n, yq in enumerate(far_y[:-1]):
        sa[n].wait_recv()
        sh_b[n] = (sh_own[n] + sh_recv_a[n].astype(F32)).astype(BF)
        sb.append(
            remote(sh_b.at[n], sh_recv_b.at[n], sb_s.at[n], sb_r.at[n], tp=yq * CORES + core)
        )

    outs = []
    for t in range(tp):
        at = pl.ds(t * share, share)
        outs.append(pltpu.make_async_copy(rx.at[t, 0], x_out.at[:, :, at], out_sem.at[2 * t]))
        outs.append(pltpu.make_async_copy(rx.at[t, 1], c_out.at[:, :, at], out_sem.at[2 * t + 1]))
    for out in outs:
        out.start()

    hidden, d_gate, d_up = activations(acc[0], acc[1], acc[2])
    hid_out[...] = hidden
    dg_out[...] = d_gate
    du_out[...] = d_up
    prod[...] = hidden.astype(F32) * acc[2]

    ra = []
    for n, yq in enumerate(far_y):
        value = part_of(yq * CORES + 1 - core, d_gate, d_up, wg, wu).astype(BF)
        part_a[n] = value.reshape(ep, cap_pad, share)
        ra.append(
            remote(part_a.at[n, :, filled], recv_a.at[n, :, filled], ra_s.at[n], ra_r.at[n], tp=mate)
        )
    rb = []
    for n, yq in enumerate(far_y):
        value = part_of(yq * CORES + core, d_gate, d_up, wg, wu)
        part_own[n] = value.reshape(ep, cap_pad, share)
        if n < ny - 1:
            ra[n].wait_recv()
            part_b[n] = (part_own[n] + recv_a[n].astype(F32)).astype(BF)
            rb.append(
                remote(
                    part_b.at[n, :, filled], recv_b.at[n, :, filled], rb_s.at[n], rb_r.at[n],
                    tp=yq * CORES + core,
                )
            )

    gpart[...] = jnp.zeros_like(gpart)
    ones = jnp.ones((8, ff), F32)
    for i in range(ep):
        gpart[i, :, :cap_pad] = lax.dot_general(
            ones, prod[i * cap_pad : (i + 1) * cap_pad, :], (((1,), (1,)), ((), ())),
            preferred_element_type=F32, precision=lax.Precision.HIGHEST,
        )
    gx = []
    for step in range(1, tp):
        gx.append(remote(gpart, grecv.at[step], g_s.at[step], g_r.at[step], tp=lax.rem(j + step, tp)))

    for copy in gx:
        copy.wait_recv()
    total = gpart[...]
    for step in range(1, tp):
        total = total + grecv[step]
    gsend[...] = total.astype(BF).astype(F32)
    gb = []
    for step in range(1, ep):
        to = ep_peer(step)
        gb.append(remote(gsend.at[to], gback.at[me], gb_s.at[step], gb_r.at[step], ep=to))
    gback[me] = gsend[me]

    ra[ny - 1].wait_recv()
    part = part_own[ny - 1] + recv_a[ny - 1].astype(F32)
    for n in range(ny - 1):
        rb[n].wait_recv()
        part = part + recv_b[n].astype(F32)
    back_tx[...] = part.astype(BF)
    bk = []
    for step in range(1, ep):
        to = ep_peer(step)
        bk.append(
            remote(
                back_tx.at[to, filled], back_rx.at[me, filled], bk_s.at[step], bk_r.at[step], ep=to
            )
        )
    back_rx[me, :live] = back_tx[me, :live]

    sa[ny - 1].wait_recv()
    shared_tot = sh_own[ny - 1] + sh_recv_a[ny - 1].astype(F32)
    for n in range(ny - 1):
        sb[n].wait_recv()
        shared_tot = shared_tot + sh_recv_b[n].astype(F32)

    norm_down = jnp.zeros((1, ff), F32)
    for t in range(tp):
        at = slice(t * share, (t + 1) * share)
        x_in = rx[t, 0].reshape(rows, share)
        c_in = rx[t, 1].reshape(rows, share)
        sq[0:1, at] = jnp.sum(jnp.square(dot(dg_out[...], x_in, 0, 0)), axis=0, keepdims=True)
        sq[1:2, at] = jnp.sum(jnp.square(dot(du_out[...], x_in, 0, 0)), axis=0, keepdims=True)
        norm_down += jnp.sum(jnp.square(dot(c_in, hid_out[...], 0, 0)), axis=0, keepdims=True)
    norm_down_out[...] = norm_down / width
    qx = []
    for step in range(1, tp):
        qx.append(remote(sq, sq_rx.at[step], q_s.at[step], q_r.at[step], tp=lax.rem(j + step, tp)))

    for copy in qx:
        copy.wait_recv()
    squares = sq[...]
    for step in range(1, tp):
        squares = squares + sq_rx[step]
    norm_in_out[...] = squares / (tp * ff)

    for copy in rp:
        copy.wait_recv()
    grad = pair_rx[0].astype(F32)
    for i in range(1, groups):
        grad = grad + pair_rx[i].astype(F32)
    shared_out[...] = grad
    norm_sh = jnp.mean(jnp.square(grad), axis=1, keepdims=True)
    here = lax.broadcasted_iota(jnp.int32, (sr, sr), 0) == lax.broadcasted_iota(
        jnp.int32, (sr, sr), 1
    )
    norm_sh_out[...] = jnp.sum(jnp.where(here, norm_sh, 0.0), axis=0, keepdims=True)

    for copy in gb:
        copy.wait_recv()
    spot = lax.broadcasted_iota(jnp.int32, (tok, 128), 1)
    spot_f = spot.astype(F32)
    for k in range(top):
        picked = jnp.zeros((tok, 128), F32)
        for i in range(ep):
            hit = (spot < cap_pad) & (slot_col[k] == spot_f + float(i * cap_pad))
            picked = picked + jnp.where(hit, gback[i, 0:1, :], 0.0)
        dots = to_row(jnp.sum(picked, axis=1, keepdims=True))
        gate_out[k : k + 1, :] = dots / gate_rows[k : k + 1, :]

    place = lax.broadcasted_iota(jnp.int32, (tok, rows), 1).astype(F32)
    pick = jnp.zeros((tok, rows), F32)
    for k in range(top):
        pick = pick + jnp.where(place == slot_col[k], 1.0, 0.0)
    for copy in bk:
        copy.wait_recv()
    token_out[...] = (
        dot(pick.astype(BF), back_rx[...].reshape(rows, share)) + shared_tot
    ).astype(BF)

    sent = rx.at[j, :, :, filled]
    for step in range(ny):
        pltpu.make_async_remote_copy(
            src_ref=sent, dst_ref=sent, send_sem=d2_s.at[step], recv_sem=d2_r.at[j],
            device_id={"tp": mate}, device_id_type=MESH,
        ).wait_send()
    for copy in waits + passed + ra + gx + rb + qx + gb + bk + rs + rp + sa + sb:
        copy.wait_send()
    for out in outs:
        out.wait()


def on_device(
    ep, tp, tokens, routes, route_gates, cotangent, w_gate, w_up, w_down, s_gate, s_up, s_down
):
    tok, width = tokens.shape
    top = routes.shape[1]
    cap = max(2, (9 * tok * top + 8 * ep - 1) // (8 * ep))
    cap_pad = -(-cap // 16) * 16
    rows, share, ff, ny = ep * cap_pad, width // tp, w_gate.shape[2], tp // CORES
    sff = s_gate.shape[1]
    sr = sff // ep

    live = -(-cap // 8) * 8

    vm, hbm = pl.BlockSpec(memory_space=pltpu.VMEM), pl.BlockSpec(memory_space=pl.ANY)
    dma, sds = pltpu.SemaphoreType.DMA, jax.ShapeDtypeStruct
    out_shape = [
        sds((tok, share), BF), sds((top, tok), F32), sds((sr, width), F32), sds((2, width), F32),
        sds((1, ff), F32), sds((1, sr), F32),
        sds((ep, cap_pad, width), BF), sds((ep, cap_pad, width), BF),
        sds((rows, ff), BF), sds((rows, ff), BF), sds((rows, ff), BF),
    ]
    slots = (ny, ep, cap_pad, share)
    scratch = [
        pltpu.VMEM((width, ff), BF), pltpu.VMEM((width, ff), BF), pltpu.VMEM((ff, width), BF),
        pltpu.VMEM((width, sff), BF), pltpu.VMEM((width, sff), BF), pltpu.VMEM((sff, width), BF),
        pltpu.VMEM((2, ep, cap_pad, share), BF),
        pltpu.VMEM((tp, 2, ep, cap_pad, share), BF),
        pltpu.VMEM((3, rows, ff), F32), pltpu.VMEM((rows, ff), F32),
        pltpu.VMEM((2, ep // 2, sr, width), BF), pltpu.VMEM((ep // 2, sr, width), BF),
        pltpu.VMEM((ep // 2, sr, width), BF), pltpu.VMEM((ep // 2, sr, width), BF),
        pltpu.VMEM(slots, BF), pltpu.VMEM(slots, F32), pltpu.VMEM(slots, BF),
        pltpu.VMEM(slots, BF), pltpu.VMEM(slots, BF),
        pltpu.VMEM((ny, tok, share), BF), pltpu.VMEM((ny, tok, share), F32),
        pltpu.VMEM((ny, tok, share), BF), pltpu.VMEM((ny, tok, share), BF),
        pltpu.VMEM((ny, tok, share), BF),
        pltpu.VMEM((ep, cap_pad, share), BF), pltpu.VMEM((ep, cap_pad, share), BF),
        pltpu.VMEM((ep, 8, 128), F32), pltpu.VMEM((tp, ep, 8, 128), F32),
        pltpu.VMEM((ep, 8, 128), F32), pltpu.VMEM((ep, 8, 128), F32),
        pltpu.VMEM((2, width), F32), pltpu.VMEM((tp, 2, width), F32),
        dma((6,)), dma((2 * tp,)), dma((ep,)), dma((ep,)), dma((ny,)), dma((tp + ny,)), dma((ny,)),
        dma((ep,)), dma((ep,)), dma((ep,)), dma((ep,)), dma((ny,)), dma((ny,)), dma((ny,)), dma((ny,)),
        dma((ep,)), dma((ep,)), dma((tp,)), dma((tp,)), dma((ep,)), dma((ep,)), dma((tp,)), dma((tp,)),
        dma((ny,)), dma((ny,)), dma((ny,)), dma((ny,)),
    ]
    out = pl.pallas_call(
        functools.partial(body, ep, tp, cap_pad, live),
        out_shape=out_shape,
        in_specs=[vm] * 4 + [hbm] * 6,
        out_specs=[vm] * 6 + [hbm] * 2 + [vm] * 3,
        scratch_shapes=scratch,
        compiler_params=pltpu.CompilerParams(
            collective_id=0, has_side_effects=True, vmem_limit_bytes=60 * 1024 * 1024
        ),
    )(
        routes.T, route_gates.T, tokens, cotangent,
        w_gate[0], w_up[0], w_down[0], s_gate, s_up, s_down,
    )
    token_grad, gate_grad, grad_shared, norm_in, norm_down, norm_sh, x, c, hid, dg, du = out
    x, c = x.reshape(rows, width), c.reshape(rows, width)
    return (
        token_grad, gate_grad.T, dot(x, dg, 0, 0)[None], dot(x, du, 0, 0)[None],
        dot(hid, c, 0, 0)[None], grad_shared, norm_in[None], norm_down.reshape(1, ff),
        norm_sh.reshape(sr),
    )


def solution(mesh):
    placed = (
        P("ep", None), P("ep", None), P("ep", None), P("ep", None),
        P("ep", None, "tp"), P("ep", None, "tp"), P("ep", "tp", None),
        P(None, "tp"), P(None, "tp"), P("tp", None),
    )
    return jax.shard_map(
        functools.partial(on_device, mesh.shape["ep"], mesh.shape["tp"]),
        mesh=mesh,
        in_specs=placed,
        out_specs=(
            P("ep", "tp"), P("ep", None), P("ep", None, "tp"), P("ep", None, "tp"),
            P("ep", "tp", None), P(("tp", "ep"), None), P("ep", None, None), P("ep", "tp"),
            P(("tp", "ep")),
        ),
        check_vma=False,
    )
```
